32 devices in a mesh: grp: 2 (over y), sp: 4 (over z), tp: 4 (over x, core).
Axes of the slice: x: 2, y: 2, z: 4, core: 2. Of those that a mesh axis runs over, the one named last changes fastest.
Arguments:
- tokens_in: bfloat16 [2048, 2048], P(('grp', 'sp'), 'tp'), parts along dimension 0, may hold values from -6 to 6
- norm_gain: float32 [3, 2048], replicated, may hold values from 0.1 to 1.9
- w_pool_in: bfloat16 [3, 2048, 1024], P(None, 'sp', 'tp'), may hold values from -0.125 to 0.125
- w_gate: bfloat16 [3, 2048, 2048], P(None, 'sp', 'tp'), may hold values from -0.125 to 0.125
- w_back: bfloat16 [3, 1024, 2048], P(None, 'tp', 'sp'), may hold values from -0.25 to 0.25
Outputs:
- tokens_out: bfloat16 [2048, 2048], P(('grp', 'sp'), 'tp'), parts along dimension 0
The draws below stay inside these ranges and needn't reach their ends.
There are 2 independent parts, one for each index of `grp`. The reference program is written for one: setup_inputs(seed, part) draws one part's arguments, and reference() takes and returns one part's arrays. A program takes and returns all parts, laid end to end along the dimension named above; an argument that names none is the same for every part. Nothing has to cross between parts.
All inputs are finite; a program needn't handle non-finite values.
Results may differ from the reference program's by a relative error of at most 0.017.
Values may be sent and summed in bfloat16 or wider, within the bound.
No kernel may reach another device: no remote copies, remote signals or barrier semaphores. Data moves between devices by JAX's collectives and lax.ppermute only.
A program may use at most 64 MiB of HBM per device.

```python
import jax
import jax.numpy as jnp
from jax import lax

D = 2048
POOL_WIDTH = 1024
GROUPS = 4
GRID_W = 32
LAYERS = 3
TOKENS = 1024
N_TP = 4


def spiked(drawn, key, source, target, blocks, factor):
    def block_of(axis_at):
        return (jnp.arange(drawn.shape[axis_at]) // (drawn.shape[axis_at] // blocks)).reshape((-1,) + (1,) * (drawn.ndim - 1 - axis_at))

    near = jax.random.permutation(key, blocks)[block_of(target)]
    second = (block_of(target) + blocks // 2) % blocks
    return jnp.where((block_of(source) == near) | (block_of(source) == second), factor * drawn, drawn)


def shard_levels(own_key, shape, shards, smallest, top_value):
    loudness = 1.0
    for axis_at, shards_of in shards:
        heights = jax.random.uniform(jax.random.fold_in(jax.random.fold_in(own_key, 6), axis_at), (shards_of,), jnp.float32, smallest / len(shards), top_value / len(shards))
        loudness = loudness * jnp.repeat(jnp.exp(heights), shape[axis_at] // shards_of).reshape((-1,) + (1,) * (len(shape) - 1 - axis_at))
    return loudness


def normal_values(rng, dims, deviation, most, cuts=(), kind=jnp.bfloat16):
    array = jax.random.normal(rng, dims, jnp.float32) * deviation
    if len(cuts) > 0:
        array = shard_levels(rng, dims, cuts, -0.22, 0.18) * array
    return jnp.clip(array, min=-most, max=most).astype(kind)


def heavy_noise(stream_key, extent, width, bound, cuts, heavy, kind=jnp.bfloat16):
    drawn = width * jax.random.normal(stream_key, extent, jnp.float32)
    if cuts:
        drawn = drawn * shard_levels(stream_key, extent, cuts, -0.22, 0.18)
    return jnp.clip(spiked(drawn, jax.random.fold_in(stream_key, 3), *heavy), -bound, bound).astype(kind)


def setup_inputs(seed: int = 0, part: int = 0) -> dict:
    arg_keys = jax.random.split(jax.random.key(seed), 6)
    part_splits = jax.random.split(jax.random.fold_in(arg_keys[5], part), 6)
    return {
        "tokens_in": normal_values(part_splits[0], (TOKENS, D), 1.0, 6.0, ((0, 4), (1, 4))),
        "norm_gain": jnp.clip(1.0 + 0.18 * jax.random.normal(arg_keys[1], (LAYERS, D), jnp.float32), 0.1, 1.9),
        "w_pool_in": normal_values(arg_keys[2], (LAYERS, D, POOL_WIDTH), D ** -0.5, 0.125, ((1, 4), (2, 4))),
        "w_gate": normal_values(arg_keys[3], (LAYERS, D, D), D ** -0.5, 0.125, ((1, 4), (2, 4))),
        "w_back": heavy_noise(arg_keys[4], (LAYERS, POOL_WIDTH, D), POOL_WIDTH ** -0.5, 0.25, ((1, 4), (2, 4)), (1, 2, 4, 2.0)),
    }


pool_windows = (2, 4, 8, 16)
norm_eps = 1e-06

def window_means(padded, rows_here, first_row, total_rows, window):
    reach = max(pool_windows) // 2
    half_span = window // 2
    width_cols = padded.shape[1] - 2 * reach
    row_sums = padded[reach - half_span:reach - half_span + rows_here]
    for offset in range(1 - half_span, half_span):
        row_sums = row_sums + padded[reach + offset:reach + offset + rows_here]
    box_sums = row_sums[:, reach - half_span:reach - half_span + width_cols]
    for offset in range(1 - half_span, half_span):
        box_sums = box_sums + row_sums[:, reach + offset:reach + offset + width_cols]
    row_index = first_row + jnp.arange(rows_here, dtype=jnp.int32)
    col_index = jnp.arange(width_cols, dtype=jnp.int32)
    row_counts = jnp.minimum(row_index + half_span, total_rows) - jnp.maximum(row_index - half_span, 0)
    col_counts = jnp.minimum(col_index + half_span, width_cols) - jnp.maximum(col_index - half_span, 0)
    counts = (row_counts[:, None] * col_counts[None, :]).astype(jnp.float32)
    return box_sums / counts[:, :, None]

def reference(tokens_in, norm_gain, w_pool_in, w_gate, w_back):
    reach = max(pool_windows) // 2
    group_width = POOL_WIDTH // GROUPS
    total_rows = TOKENS // GRID_W
    block_width = POOL_WIDTH // N_TP
    state = tokens_in
    for layer_id in range(LAYERS):
        wide = state.astype(jnp.float32)
        normed = (wide * lax.rsqrt(lax.optimization_barrier(jnp.mean(wide * wide, axis=-1, keepdims=True)) + norm_eps) * norm_gain[layer_id]).astype(jnp.bfloat16)
        pool_in = jnp.dot(normed, w_pool_in[layer_id], preferred_element_type=jnp.float32).astype(jnp.bfloat16)
        gate = jax.nn.sigmoid(jnp.dot(normed, w_gate[layer_id], preferred_element_type=jnp.float32))
        cells = pool_in.astype(jnp.float32).reshape(total_rows, GRID_W, POOL_WIDTH)
        padded = jnp.pad(cells, ((reach, reach), (reach, reach), (0, 0)))
        pieces = []
        for group_id in range(GROUPS):
            chosen = padded[:, :, group_id * group_width:(group_id + 1) * group_width]
            pieces.append(window_means(chosen, total_rows, 0, total_rows, pool_windows[group_id]))
        means = jnp.concatenate(pieces, axis=2)
        pooled = (means - cells).reshape(TOKENS, POOL_WIDTH).astype(jnp.bfloat16)
        branch = jnp.zeros((TOKENS, D), jnp.float32)
        for block_id in range(N_TP):
            lower = block_id * block_width
            partial_value = jnp.dot(pooled[:, lower:lower + block_width], w_back[layer_id][lower:lower + block_width], preferred_element_type=jnp.float32).astype(jnp.bfloat16)
            branch = branch + lax.optimization_barrier(partial_value).astype(jnp.float32)
        state = (wide + gate * branch).astype(jnp.bfloat16)
    return state
```

```python
import jax
import jax.numpy as jnp
from jax import lax
from jax.experimental import pallas as pl
from jax.experimental.pallas import tpu as pltpu
from jax.sharding import PartitionSpec as P

POOL_WIDTH = 1024
GROUPS = 4
GRID_W = 32
LAYERS = 3


pool_windows = (2, 4, 8, 16)
norm_eps = 1e-06


def padded_2(value, sides, width):
    for axis, dim in sides:
        peers, length = (lax.axis_size(axis), value.shape[dim])
        up = [(i, (i + 1) % peers) for i in range(peers - 1)]
        down = [(j, i) for i, j in up]
        last = lax.slice_in_dim(value, length - width, length, axis=dim)
        initial = lax.slice_in_dim(value, 0, width, axis=dim)
        before = lax.ppermute(last, axis, up)
        after = lax.ppermute(initial, axis, down)
        value = jnp.concatenate([before, value, after], axis=dim)
    return value


def window_means(padded, rows_here, first_row, total_rows, window):
    reach = max(pool_windows) // 2
    half_span = window // 2
    width_cols = padded.shape[1] - 2 * reach
    row_sums = padded[reach - half_span : reach - half_span + rows_here]
    for offset in range(1 - half_span, half_span):
        row_sums = row_sums + padded[reach + offset : reach + offset + rows_here]
    box_sums = row_sums[:, reach - half_span : reach - half_span + width_cols]
    for offset in range(1 - half_span, half_span):
        box_sums = box_sums + row_sums[:, reach + offset : reach + offset + width_cols]
    row_index = first_row + jnp.arange(rows_here, dtype=jnp.int32)
    col_index = jnp.arange(width_cols, dtype=jnp.int32)
    row_counts = jnp.minimum(row_index + half_span, total_rows) - jnp.maximum(
        row_index - half_span, 0
    )
    col_counts = jnp.minimum(col_index + half_span, width_cols) - jnp.maximum(
        col_index - half_span, 0
    )
    counts = (row_counts[:, None] * col_counts[None, :]).astype(jnp.float32)
    return box_sums / counts[:, :, None]


def by_gathers(tokens_in, norm_gain, w_pool_in, w_gate, w_back):
    reach = max(pool_windows) // 2
    sp_count = lax.axis_size("sp")
    tp_count = lax.axis_size("tp")
    tp_pos = lax.axis_index("tp")
    sp_pos = lax.axis_index("sp")
    tok_rows = tokens_in.shape[0]
    rows_here = tok_rows // GRID_W
    total_rows = rows_here * sp_count
    first_row = sp_pos * rows_here
    local_pool = w_pool_in.shape[2]
    group_width = POOL_WIDTH // GROUPS
    channel_group = (tp_pos * local_pool + jnp.arange(local_pool, dtype=jnp.int32)) // group_width
    state = tokens_in
    for layer_id in range(LAYERS):
        whole_rows = lax.all_gather(state, "tp", axis=1, tiled=True)
        wide = whole_rows.astype(jnp.float32)
        normed = (
            wide
            * lax.rsqrt(jnp.mean(wide * wide, axis=-1, keepdims=True) + norm_eps)
            * norm_gain[layer_id]
        ).astype(jnp.bfloat16)
        pool_acc = jnp.dot(
            normed,
            lax.all_gather(w_pool_in[layer_id], "sp", axis=0, tiled=True),
            preferred_element_type=jnp.float32,
        )
        gate_acc = jnp.dot(
            normed,
            lax.all_gather(w_gate[layer_id], "sp", axis=0, tiled=True),
            preferred_element_type=jnp.float32,
        )
        pool_in = pool_acc.astype(jnp.bfloat16)
        gate = jax.nn.sigmoid(gate_acc)
        cells = pool_in.reshape(rows_here, GRID_W, local_pool)
        rimmed = padded_2(cells, (("sp", 0),), reach)
        padded = jnp.pad(rimmed.astype(jnp.float32), ((0, 0), (reach, reach), (0, 0)))
        means = jnp.zeros((rows_here, GRID_W, local_pool), jnp.float32)
        for group_id in range(GROUPS):
            in_group = (channel_group == group_id)[None, None, :]
            means = jnp.where(
                in_group,
                window_means(padded, rows_here, first_row, total_rows, pool_windows[group_id]),
                means,
            )
        pooled = (
            (means - cells.astype(jnp.float32)).reshape(tok_rows, local_pool).astype(jnp.bfloat16)
        )
        full_pooled = lax.all_gather(pooled, "tp", axis=1, tiled=True)
        back_rows = lax.all_gather(w_back[layer_id], "sp", axis=1, tiled=True)
        back_cols = lax.all_to_all(back_rows, "tp", split_axis=1, concat_axis=0, tiled=True)
        partials = jnp.einsum(
            "tnb,nbd->ntd",
            full_pooled.reshape(tok_rows, tp_count, local_pool),
            back_cols.reshape(tp_count, local_pool, back_cols.shape[1]),
            preferred_element_type=jnp.float32,
        ).astype(jnp.bfloat16)
        branch = jnp.sum(partials.astype(jnp.float32), axis=0)
        state = (state.astype(jnp.float32) + gate * branch).astype(jnp.bfloat16)
    return state


BF16 = jnp.bfloat16
F32 = jnp.float32


def swapped(value, axis, distance):
    count = lax.axis_size(axis)
    return lax.ppermute(value, axis, [(i, i ^ distance) for i in range(count)])


def fetched(shard):
    count = lax.axis_size("sp")
    way = [(s, (s + 1) % count) for s in range(count)]
    way += [(count + s, count + (s - 1) % count) for s in range(count)]
    first = lax.ppermute(shard, ("grp", "sp"), way)
    first_swapped = swapped(first, "grp", 1)
    half = lax.dynamic_index_in_dim(first, lax.axis_index("grp"), 0, keepdims=False)
    second = lax.ppermute(half, ("grp", "sp"), way)
    second_swapped = swapped(second, "grp", 1)
    return shard, first, first_swapped, second, second_swapped


def shard_dots(left, sp_pos, grp_pos, pieces, rows):
    own, first, first_swapped, second, second_swapped = pieces
    before = (sp_pos + 3 + 2 * grp_pos) % 4
    after = (sp_pos + 1 + 2 * grp_pos) % 4
    across = (sp_pos + 2) % 4

    def dot(block, weight):
        return jnp.dot(left[block], weight, preferred_element_type=F32)

    total = dot(2 * sp_pos, own[0, :rows]) + dot(2 * sp_pos + 1, own[1, :rows])
    total += dot(2 * before, first[0, :rows]) + dot(2 * before + 1, first[1, :rows])
    total += dot(2 * after, first_swapped[0, :rows]) + dot(2 * after + 1, first_swapped[1, :rows])
    total += dot(2 * across + grp_pos, second[:rows])
    total += dot(2 * across + 1 - grp_pos, second_swapped[:rows])
    return total


def norm_pool_kernel(place, same, other, gain, own, first, first_swapped, second, second_swapped, normed, pool_in):
    sp_pos, grp_pos, core = place[0], place[1], place[2]
    rows, width = same.shape[1:]
    squares = jnp.zeros((rows, width), F32)
    for part in (same, other):
        for p in range(2):
            wide = part[p].astype(F32)
            squares += wide * wide
    scale = lax.rsqrt(jnp.sum(squares, axis=-1, keepdims=True) / (4 * width) + norm_eps)
    for part, parity in ((same, core), (other, 1 - core)):
        for p in range(2):
            block = 2 * p + parity
            value = (part[p].astype(F32) * scale * gain[block]).astype(BF16)
            normed[2 * block] = value[:, : width // 2]
            normed[2 * block + 1] = value[:, width // 2 :]
    pieces = (own, first, first_swapped, second, second_swapped)
    pool_in[...] = shard_dots(normed, sp_pos, grp_pos, pieces, own.shape[1]).astype(BF16)


def gate_kernel(place, normed, own, first, first_swapped, second, second_swapped, gate):
    pieces = (own, first, first_swapped, second, second_swapped)
    total = shard_dots(normed, place[0], place[1], pieces, normed.shape[2])
    gate[...] = jax.nn.sigmoid(total).astype(gate.dtype)


def back_kernel(
    place, masks, counts, rows_before, cells, rows_after, own, first, first_swapped, second, second_swapped,
    kept, sent, across_rows, partials,
):
    sp_pos, grp_pos, core = place[0], place[1], place[2]
    skip = own.shape[1] - cells.shape[1] // 2
    sums = jnp.dot(masks[1], cells[...], preferred_element_type=F32)
    sums += jnp.dot(masks[0], rows_before[...], preferred_element_type=F32)
    sums += jnp.dot(masks[2], rows_after[...], preferred_element_type=F32)
    pooled = (sums / counts[...] - cells[...].astype(F32)).astype(BF16)
    across_rows[grp_pos] = second[skip:]
    across_rows[1 - grp_pos] = second_swapped[skip:]

    def put(shard, upper, lower):
        weight = jnp.concatenate([upper, lower], axis=0)
        partials[shard] = jnp.dot(pooled, weight, preferred_element_type=F32).astype(BF16)

    put(sp_pos, own[0, skip:], own[1, skip:])
    put((sp_pos + 3 + 2 * grp_pos) % 4, first[0, skip:], first[1, skip:])
    put((sp_pos + 1 + 2 * grp_pos) % 4, first_swapped[0, skip:], first_swapped[1, skip:])
    put((sp_pos + 2) % 4, across_rows[0], across_rows[1])
    for p in range(2):
        kept[p] = partials[2 * p + core]
        sent[p] = partials[2 * p + 1 - core]


def call(kernel, outs, place, *operands, scratch=()):
    vmem = pl.BlockSpec(memory_space=pltpu.VMEM)
    return pl.pallas_call(
        kernel,
        out_shape=outs,
        in_specs=[pl.BlockSpec(memory_space=pltpu.SMEM)] + [vmem] * len(operands),
        out_specs=[vmem] * len(outs),
        scratch_shapes=scratch,
        compiler_params=pltpu.CompilerParams(vmem_limit_bytes=40 * 1024 * 1024),
    )(place, *operands)


def box_masks(half_span, rows_here, reach, first_row, total_rows):
    here = jnp.arange(rows_here * GRID_W, dtype=jnp.int32)
    span = max(rows_here, reach)
    row, col = here // GRID_W, here % GRID_W

    def mask(source_row, source_col):
        down = source_row[None, :] - row[:, None]
        right = source_col[None, :] - col[:, None]
        inside = (down >= -half_span) & (down < half_span) & (right >= -half_span) & (right < half_span)
        return inside.astype(BF16)

    near = jnp.arange(reach * GRID_W, dtype=jnp.int32)
    masks = jnp.stack(
        [
            mask(near // GRID_W - reach, near % GRID_W),
            mask(row, col),
            mask(near // GRID_W + rows_here, near % GRID_W),
        ]
    )
    row = row + first_row
    row_counts = jnp.minimum(row + half_span, total_rows) - jnp.maximum(row - half_span, 0)
    col_counts = jnp.minimum(col + half_span, GRID_W) - jnp.maximum(col - half_span, 0)
    return masks, (row_counts * col_counts).astype(F32)[:, None]


def by_permutes(tokens_in, norm_gain, w_pool_in, w_gate, w_back):
    reach = max(pool_windows) // 2
    sp_count, tp_count = lax.axis_size("sp"), lax.axis_size("tp")
    grp_pos, sp_pos, tp_pos = lax.axis_index("grp"), lax.axis_index("sp"), lax.axis_index("tp")
    side, core = tp_pos // 2, tp_pos % 2
    place = jnp.stack([sp_pos, grp_pos, core]).astype(jnp.int32)
    tok_rows, width = tokens_in.shape
    rows_here = tok_rows // GRID_W
    local_pool = w_pool_in.shape[2]
    group_id = tp_pos * local_pool // (POOL_WIDTH // GROUPS)
    half_span = jnp.asarray(pool_windows, jnp.int32)[group_id] // 2
    up = [(i, i + 1) for i in range(sp_count - 1)]
    down = [(j, i) for i, j in up]
    halves = 2

    def split(value):
        return value.reshape(halves, value.shape[0] // halves, value.shape[1])

    def both_sides(mine, theirs):
        return jnp.where(side == 0, jnp.stack([mine, theirs]), jnp.stack([theirs, mine]))

    pools, rests = [], []
    for layer_id in range(LAYERS):
        pools.append(fetched(split(w_pool_in[layer_id])))
        rests.append(fetched(jnp.concatenate([split(w_gate[layer_id]), split(w_back[layer_id])], axis=1)))
    gains = norm_gain.reshape(LAYERS, sp_count, 1, width)
    masks, counts = box_masks(half_span, rows_here, reach, sp_pos * rows_here, rows_here * sp_count)

    state = both_sides(tokens_in, swapped(tokens_in, "tp", 2))
    for layer_id in range(LAYERS):
        other = swapped(state, "tp", 1)
        normed, pool_in = call(
            norm_pool_kernel,
            [
                jax.ShapeDtypeStruct((halves * sp_count, tok_rows, width // halves), BF16),
                jax.ShapeDtypeStruct((tok_rows, local_pool), BF16),
            ],
            place, state, other, gains[layer_id], *pools[layer_id],
        )
        near = reach * GRID_W
        rows_before = lax.ppermute(pool_in[tok_rows - near :], "sp", up)
        rows_after = lax.ppermute(pool_in[:near], "sp", down)
        (gate,) = call(
            gate_kernel,
            [jax.ShapeDtypeStruct((tok_rows, width), BF16)],
            place, normed, *rests[layer_id],
        )
        last = layer_id + 1 == LAYERS
        if not last:
            gate = both_sides(gate, swapped(gate, "tp", 2))
        kept, sent = call(
            back_kernel,
            [jax.ShapeDtypeStruct((2, tok_rows, width), BF16)] * 2,
            place, masks, counts, rows_before, pool_in, rows_after, *rests[layer_id],
            scratch=(
                pltpu.VMEM((2, local_pool // 2, width), BF16),
                pltpu.VMEM((sp_count, tok_rows, width), BF16),
            ),
        )
        chip_sum = (kept.astype(F32) + swapped(sent, "tp", 1).astype(F32)).astype(BF16)
        if last:
            mine = lax.dynamic_index_in_dim(chip_sum, side, 0, keepdims=False)
            theirs = swapped(lax.dynamic_index_in_dim(chip_sum, 1 - side, 0, keepdims=False), "tp", 2)
            state = lax.dynamic_index_in_dim(state, side, 0, keepdims=False)
        else:
            mine, theirs = chip_sum, swapped(chip_sum, "tp", 2)
        branch = mine.astype(F32) + theirs.astype(F32)
        state = (state.astype(F32) + gate.astype(F32) * branch).astype(BF16)
    return state


def body_for(mesh):
    sizes = dict(mesh.shape)
    if (sizes["grp"], sizes["sp"], sizes["tp"]) == (2, 4, 4):
        return by_permutes
    return by_gathers


def solution(mesh):
    return jax.shard_map(
        body_for(mesh),
        mesh=mesh,
        in_specs=(
            P(("grp", "sp"), "tp"),
            P(),
            P(None, "sp", "tp"),
            P(None, "sp", "tp"),
            P(None, "tp", "sp"),
        ),
        out_specs=P(("grp", "sp"), "tp"),
        check_vma=False,
    )
```
